32 devices in a mesh: rep: 4 (over z), fs: 4 (over y, x), tp: 2 (over core).
Axes of the slice: x: 2, y: 2, z: 4, core: 2. Of those that a mesh axis runs over, the one named last changes fastest.
Arguments:
- tokens: bfloat16 [16, 768, 2048], P(('rep', 'fs')), may hold values from -6 to 6
- norm_gain: float32 [2048], replicated, may hold values from 0.1 to 1.9
- outer_weight: bfloat16 [2048, 2048], P('fs', 'tp'), may hold values from -0.125 to 0.125
- inner_weight: bfloat16 [2048, 2048], P('fs', 'tp'), may hold values from -0.125 to 0.125
- value_weight: bfloat16 [2048, 2048], P('fs', 'tp'), may hold values from -0.125 to 0.125
- conv_taps: float32 [3, 2048], replicated, may hold values from -3.5 to 3.5
- out_weight: bfloat16 [2048, 2048], P('fs', 'tp'), may hold values from -0.125 to 0.125
Outputs:
- mixed: bfloat16 [16, 768, 2048], P(('rep', 'fs'), None, 'tp')
The draws below stay inside these ranges and needn't reach their ends.
All inputs are finite; a program needn't handle non-finite values.
Results may differ from the reference program's by a relative error of at most 0.014.
Values may be sent and summed in bfloat16 or wider, within the bound.
A program may use at most 64 MiB of HBM per device.

```python
import jax
import jax.numpy as jnp
from jax import lax

D = 2048
TAPS = 3
SEQ = 768
BATCH = 16


def steps_of(rng, dims, cuts, least, top_value):
    level = 1.0
    for axis_at, parts in cuts:
        heights = jax.random.uniform(jax.random.fold_in(jax.random.fold_in(rng, 6), axis_at), (parts,), jnp.float32, least / len(cuts), top_value / len(cuts))
        level = level * jnp.repeat(jnp.exp(heights), dims[axis_at] // parts).reshape((-1,) + (1,) * (len(dims) - 1 - axis_at))
    return level


def bell_draw(key, extent, deviation, limit, cuts=(), kind=jnp.bfloat16):
    array = deviation * jax.random.normal(key, extent, jnp.float32)
    if cuts:
        array = array * steps_of(key, extent, cuts, -0.22, 0.18)
    return jnp.clip(array, -limit, limit).astype(kind)


def setup_inputs(seed: int = 0) -> dict:
    seeds = jax.random.split(jax.random.key(seed), 8)
    tokens = bell_draw(seeds[0], (BATCH, SEQ, D), 1.0, 6.0, ((0, 16),))
    norm_gain = jnp.clip(1.0 + 0.18 * jax.random.normal(seeds[1], (D,), jnp.float32), 0.1, 1.9)
    outer_weight = bell_draw(seeds[2], (D, D), D ** -0.5, 0.125, ((0, 4), (1, 2)))
    inner_weight = bell_draw(seeds[3], (D, D), D ** -0.5, 0.125, ((0, 4), (1, 2)))
    value_weight = bell_draw(seeds[4], (D, D), D ** -0.5, 0.125, ((0, 4), (1, 2)))
    conv_taps = bell_draw(seeds[5], (TAPS, D), TAPS ** -0.5, 3.5, (), jnp.float32)
    out_weight = bell_draw(seeds[6], (D, D), D ** -0.5, 0.125, ((0, 4), (1, 2)))
    return {"tokens": tokens, "norm_gain": norm_gain, "outer_weight": outer_weight, "inner_weight": inner_weight, "value_weight": value_weight, "conv_taps": conv_taps, "out_weight": out_weight}


def reference(tokens, norm_gain, outer_weight, inner_weight, value_weight, conv_taps, out_weight):
    xf = tokens.astype(jnp.float32)
    scale = lax.rsqrt(lax.optimization_barrier(jnp.mean(xf * xf, axis=-1, keepdims=True)) + 1e-06)
    normed = (xf * scale * norm_gain).astype(jnp.bfloat16)
    rows = normed.reshape(BATCH * SEQ, D)
    outer = jnp.dot(rows, outer_weight, preferred_element_type=jnp.float32).astype(jnp.bfloat16)
    inner = jnp.dot(rows, inner_weight, preferred_element_type=jnp.float32).astype(jnp.bfloat16)
    value = jnp.dot(rows, value_weight, preferred_element_type=jnp.float32).astype(jnp.bfloat16)
    product = (inner.astype(jnp.float32) * value.astype(jnp.float32)).reshape(BATCH, SEQ, D)
    padded = jnp.pad(product, ((0, 0), (TAPS - 1, 0), (0, 0)))
    convolved = jnp.zeros((BATCH, SEQ, D), jnp.float32)
    for k in range(TAPS):
        convolved = convolved + conv_taps[k] * padded[:, k:k + SEQ, :]
    gated = (outer.astype(jnp.float32) * convolved.reshape(BATCH * SEQ, D)).astype(jnp.bfloat16)
    total = jnp.dot(gated, out_weight, preferred_element_type=jnp.float32)
    return total.astype(jnp.bfloat16).reshape(BATCH, SEQ, D)
```

```python
import functools

import jax
import jax.numpy as jnp
from jax import lax
from jax.experimental import pallas as pl
from jax.experimental.pallas import tpu as pltpu
from jax.sharding import PartitionSpec as P

MESH = pl.DeviceIdType.MESH
F32 = jnp.float32
BF16 = jnp.bfloat16


def plain(tokens, norm_gain, outer_weight, inner_weight, value_weight, conv_taps, out_weight):
    batch, seq_len, width = tokens.shape
    xf = tokens.astype(F32)
    scale = lax.rsqrt(jnp.mean(xf * xf, axis=-1, keepdims=True) + 1e-06)
    normed = (xf * scale * norm_gain).astype(BF16).reshape(batch * seq_len, width)
    columns = outer_weight.shape[1]

    def project(weight):
        full = lax.all_gather(weight, "fs", axis=0, tiled=True)
        return jnp.dot(normed, full, preferred_element_type=F32).astype(BF16).astype(F32)

    outer, inner, value = project(outer_weight), project(inner_weight), project(value_weight)
    product = (inner * value).reshape(batch, seq_len, columns)
    offset = lax.axis_index("tp") * columns
    taps = lax.dynamic_slice_in_dim(conv_taps, offset, columns, 1)
    count = conv_taps.shape[0]
    padded = jnp.pad(product, ((0, 0), (count - 1, 0), (0, 0)))
    convolved = jnp.zeros((batch, seq_len, columns), F32)
    for k in range(count):
        convolved = convolved + taps[k] * padded[:, k : k + seq_len, :]
    gated = (outer * convolved.reshape(batch * seq_len, columns)).astype(BF16)
    everything = lax.all_gather(gated, "tp", axis=1, tiled=True)
    full = lax.all_gather(out_weight, "fs", axis=0, tiled=True)
    result = jnp.dot(everything, full, preferred_element_type=F32)
    return result.astype(BF16).reshape(batch, seq_len, columns)


def kernel(
    tok_hbm, gain_ref, outer_hbm, inner_hbm, value_hbm, taps_ref, outw_hbm, out_ref,
    tok, nm, wts, outw, acc, prod, gat, mine, osum, send_sems, recv_sems, local_sems,
):
    rep, fs, tp = lax.axis_index("rep"), lax.axis_index("fs"), lax.axis_index("tp")
    seq, width = tok_hbm.shape
    rows, cols = outer_hbm.shape
    half = cols // 2
    hrows = rows // 2
    count = taps_ref.shape[0]
    par = lax.rem(rep, 2)
    fx = fs + 1 - 2 * lax.rem(fs, 2)
    fy = lax.rem(fs + 2, 4)
    fd = 3 - fs
    shard = (fs, fx, fy, fd)
    to_x, to_y = (rep, fx, tp), (rep, fy, tp)
    to_z, to_t = (rep + 1 - 2 * par, fs, tp), (rep, fs, 1 - tp)
    used = [0]

    def remote(src, dst, device):
        k = used[0]
        used[0] += 1
        return pltpu.make_async_remote_copy(
            src_ref=src, dst_ref=dst, send_sem=send_sems.at[k], recv_sem=recv_sems.at[k],
            device_id=device, device_id_type=MESH,
        )

    barrier = pltpu.get_barrier_semaphore()
    for peer in (to_x, to_y, to_z, to_t):
        pl.semaphore_signal(barrier, inc=1, device_id=peer, device_id_type=MESH)

    hbm = (inner_hbm, value_hbm, outer_hbm)
    mycols = pl.ds(pl.multiple_of(par * half, half), half)
    loads = [pltpu.make_async_copy(tok_hbm, tok.at[0], local_sems.at[0])]
    for w in range(3):
        loads.append(pltpu.make_async_copy(hbm[w].at[:, mycols], wts.at[w, 0], local_sems.at[1 + w]))
    loads.append(pltpu.make_async_copy(outw_hbm, outw.at[0], local_sems.at[4]))
    for c in loads:
        c.start()

    chunks = 2
    crow = seq // 2 // chunks
    trow = [pl.ds(pl.multiple_of(tp * (seq // 2) + c * crow, 8), crow) for c in range(chunks)]
    tok_z = [remote(tok_hbm.at[r], tok.at[1, r], to_z) for r in trow]
    tok_t = [remote(tok.at[1, r], tok.at[1, r], to_t) for r in trow]
    w_x = [remote(hbm[w].at[:, mycols], wts.at[w, 1], to_x) for w in range(3)]
    w_y = [remote(hbm[w].at[:, mycols], wts.at[w, 2], to_y) for w in range(3)]
    low, high = pl.ds(0, hrows), pl.ds(hrows, hrows)
    d_x = [remote(wts.at[w, 2, low], wts.at[w, 3, low], to_x) for w in range(3)]
    d_y = [remote(wts.at[w, 1, high], wts.at[w, 3, high], to_y) for w in range(3)]
    o_x = [remote(outw_hbm.at[r], outw.at[1, r], to_x) for r in (high, low)]
    o_y = [remote(outw_hbm.at[r], outw.at[2, r], to_y) for r in (low, high)]
    od_x = remote(outw.at[2, low], outw.at[3, low], to_x)
    od_y = remote(outw.at[1, high], outw.at[3, high], to_y)
    group = tp * 2 + par
    other = tp * 2 + 1 - par
    g_z = remote(mine, gat.at[group], to_z)
    g_t = remote(gat.at[group], gat.at[group], to_t)
    g_f = remote(gat.at[other], gat.at[other], to_t)

    pl.semaphore_wait(barrier, 4)
    for w in range(3):
        w_x[w].start()
        w_y[w].start()
        if w < chunks:
            tok_z[w].start()

    tile = 128

    def norm(s):
        @pl.loop(0, seq // tile)
        def _(b):
            r = pl.multiple_of(b * tile, tile)
            xf = tok[s, pl.ds(r, tile), :].astype(F32)
            scale = lax.rsqrt(jnp.mean(xf * xf, axis=-1, keepdims=True) + 1e-06)
            y = (xf * scale * gain_ref[...]).astype(BF16)
            for j in range(4):
                nm[j, pl.ds(s * seq + r, tile), :] = y[:, j * rows : (j + 1) * rows]

    mt = 256

    def project(w, slots, start, length, fresh):
        @pl.loop(0, length // mt)
        def _(b):
            r = pl.ds(pl.multiple_of(start + b * mt, mt), mt)
            total = None
            for s in slots:
                d = jnp.dot(nm[shard[s], r, :], wts[w, s], preferred_element_type=F32)
                total = d if total is None else total + d
            if fresh:
                acc[w, r, :] = total
            else:
                acc[w, r, :] += total

    loads[0].wait()
    norm(0)
    for w in range(3):
        loads[1 + w].wait()
    loads[4].wait()
    for w in range(3):
        project(w, (0,), 0, seq, True)
    for w in range(3):
        w_y[w].wait_recv()
        d_x[w].start()
        w_x[w].wait_recv()
        d_y[w].start()
        if w == 2:
            for h in range(2):
                o_x[h].start()
                o_y[h].start()
        if w >= 1:
            tok_z[w - 1].wait_recv()
            tok_t[w - 1].start()
        project(w, (1, 2), 0, seq, False)
    tok_t[0].wait_recv()
    tok_t[1].wait_recv()
    norm(1)
    for w in range(3):
        project(w, (0, 1, 2), seq, seq, True)
    for w in range(3):
        d_x[w].wait_recv()
        d_y[w].wait_recv()
        project(w, (3,), 0, 2 * seq, False)

    tcols = pl.ds(pl.multiple_of(tp * cols + par * half, half), half)
    prod[0:8, :] = jnp.zeros((8, half), F32)

    def gate(s, store):
        @pl.loop(0, seq // tile)
        def _(b):
            r = pl.multiple_of(b * tile, tile)
            a = pl.ds(s * seq + r, tile)
            inner = acc[0, a, :].astype(BF16).astype(F32)
            value = acc[1, a, :].astype(BF16).astype(F32)
            outer = acc[2, a, :].astype(BF16).astype(F32)
            prod[pl.ds(r + 8, tile), :] = inner * value
            window = prod[pl.ds(r, tile + 8), :]
            conv = jnp.zeros((tile, half), F32)
            for k in range(count):
                lo = 8 - (count - 1) + k
                conv = conv + taps_ref[k : k + 1, tcols] * window[lo : lo + tile, :]
            store(pl.ds(r, tile), (outer * conv).astype(BF16))

    def keep_partner(r, x):
        mine[r, :] = x

    def keep_own(r, x):
        gat[group, r, :] = x

    gate(1, keep_partner)
    gate(0, keep_own)
    g_z.start()
    o_y[0].wait_recv()
    od_x.start()
    o_x[0].wait_recv()
    od_y.start()
    g_t.start()
    g_z.wait_recv()
    g_f.start()
    o_y[1].wait_recv()
    o_x[1].wait_recv()
    g_t.wait_recv()
    g_f.wait_recv()

    @pl.loop(0, seq // mt)
    def _(b):
        r = pl.ds(pl.multiple_of(b * mt, mt), mt)
        total = None
        for s in range(3):
            d = jnp.dot(gat[shard[s], r, :], outw[s], preferred_element_type=F32)
            total = d if total is None else total + d
        osum[r, :] = total

    od_x.wait_recv()
    od_y.wait_recv()

    @pl.loop(0, seq // mt)
    def _(b):
        r = pl.ds(pl.multiple_of(b * mt, mt), mt)
        d = jnp.dot(gat[fd, r, :], outw[3], preferred_element_type=F32)
        out_ref[r, :] = (osum[r, :] + d).astype(BF16)

    for c in tok_z + tok_t + w_x + w_y + d_x + d_y + o_x + o_y + [od_x, od_y, g_z, g_t, g_f]:
        c.wait_send()


COPIES = 25


def paired(tokens, norm_gain, outer_weight, inner_weight, value_weight, conv_taps, out_weight):
    _, seq, width = tokens.shape
    rows, cols = outer_weight.shape
    half = cols // 2
    anyspace = pl.BlockSpec(memory_space=pl.ANY)
    vmem = pl.BlockSpec(memory_space=pltpu.VMEM)
    out = pl.pallas_call(
        kernel,
        out_shape=jax.ShapeDtypeStruct((seq, cols), BF16),
        in_specs=[anyspace, vmem, anyspace, anyspace, anyspace, vmem, anyspace],
        out_specs=vmem,
        scratch_shapes=[
            pltpu.VMEM((2, seq, width), BF16),
            pltpu.VMEM((4, 2 * seq, rows), BF16),
            pltpu.VMEM((3, 4, rows, half), BF16),
            pltpu.VMEM((4, rows, cols), BF16),
            pltpu.VMEM((3, 2 * seq, half), F32),
            pltpu.VMEM((seq + 8, half), F32),
            pltpu.VMEM((4, seq, half), BF16),
            pltpu.VMEM((seq, half), BF16),
            pltpu.VMEM((seq, cols), F32),
            pltpu.SemaphoreType.DMA((COPIES,)),
            pltpu.SemaphoreType.DMA((COPIES,)),
            pltpu.SemaphoreType.DMA((5,)),
        ],
        compiler_params=pltpu.CompilerParams(
            collective_id=0, has_side_effects=True, vmem_limit_bytes=60 * 1024 * 1024
        ),
        name="mixer",
    )(
        tokens.reshape(seq, width), norm_gain.reshape(1, width), outer_weight, inner_weight,
        value_weight, conv_taps, out_weight,
    )
    return out.reshape(1, seq, cols)


def solution(mesh):
    shape = dict(mesh.shape)

    def local(tokens, *rest):
        rows, cols = rest[1].shape
        fits = (
            shape["fs"] == 4 and shape["tp"] == 2 and shape["rep"] % 2 == 0
            and tokens.shape[0] == 1 and tokens.shape[1] % 256 == 0
            and rows % 256 == 0 and cols == 2 * rows and rest[4].shape[0] <= 9
        )
        return (paired if fits else plain)(tokens, *rest)

    in_specs = (
        P(("rep", "fs"), None, None),
        P(),
        P("fs", "tp"),
        P("fs", "tp"),
        P("fs", "tp"),
        P(),
        P("fs", "tp"),
    )
    out_specs = P(("rep", "fs"), None, "tp")
    return jax.shard_map(local, mesh=mesh, in_specs=in_specs, out_specs=out_specs, check_vma=False)
```

```python
import functools

import jax
import jax.numpy as jnp
from jax import lax
from jax.experimental import pallas as pl
from jax.experimental.pallas import tpu as pltpu
from jax.sharding import PartitionSpec as P

MESH = pl.DeviceIdType.MESH
F32 = jnp.float32
BF16 = jnp.bfloat16


def plain(tokens, norm_gain, outer_weight, inner_weight, value_weight, conv_taps, out_weight):
    batch, seq_len, width = tokens.shape
    xf = tokens.astype(F32)
    scale = lax.rsqrt(jnp.mean(xf * xf, axis=-1, keepdims=True) + 1e-06)
    normed = (xf * scale * norm_gain).astype(BF16).reshape(batch * seq_len, width)
    columns = outer_weight.shape[1]

    def project(weight):
        full = lax.all_gather(weight, "fs", axis=0, tiled=True)
        return jnp.dot(normed, full, preferred_element_type=F32).astype(BF16).astype(F32)

    outer, inner, value = project(outer_weight), project(inner_weight), project(value_weight)
    product = (inner * value).reshape(batch, seq_len, columns)
    offset = lax.axis_index("tp") * columns
    taps = lax.dynamic_slice_in_dim(conv_taps, offset, columns, 1)
    count = conv_taps.shape[0]
    padded = jnp.pad(product, ((0, 0), (count - 1, 0), (0, 0)))
    convolved = jnp.zeros((batch, seq_len, columns), F32)
    for k in range(count):
        convolved = convolved + taps[k] * padded[:, k : k + seq_len, :]
    gated = (outer * convolved.reshape(batch * seq_len, columns)).astype(BF16)
    everything = lax.all_gather(gated, "tp", axis=1, tiled=True)
    full = lax.all_gather(out_weight, "fs", axis=0, tiled=True)
    result = jnp.dot(everything, full, preferred_element_type=F32)
    return result.astype(BF16).reshape(batch, seq_len, columns)


def kernel(
    tok_hbm, gain_ref, outer_hbm, inner_hbm, value_hbm, taps_ref, outw_hbm, out_ref,
    tok, nm, wts, outw, acc, prod, gat, mine, osum, send_sems, recv_sems, local_sems,
):
    rep, fs, tp = lax.axis_index("rep"), lax.axis_index("fs"), lax.axis_index("tp")
    seq, width = tok_hbm.shape
    rows, cols = outer_hbm.shape
    half = cols // 2
    part = half // PARTS
    hrows = rows // 2
    count = taps_ref.shape[0]
    par = lax.rem(rep, 2)
    fx = fs + 1 - 2 * lax.rem(fs, 2)
    fy = lax.rem(fs + 2, 4)
    fd = 3 - fs
    shard = (fs, fx, fy, fd)
    to_x, to_y = (rep, fx, tp), (rep, fy, tp)
    to_z, to_t = (rep + 1 - 2 * par, fs, tp), (rep, fs, 1 - tp)
    used = [0]

    def remote(src, dst, device):
        k = used[0]
        used[0] += 1
        return pltpu.make_async_remote_copy(
            src_ref=src, dst_ref=dst, send_sem=send_sems.at[k], recv_sem=recv_sems.at[k],
            device_id=device, device_id_type=MESH,
        )

    barrier = pltpu.get_barrier_semaphore()
    for peer in (to_x, to_y, to_z, to_t):
        pl.semaphore_signal(barrier, inc=1, device_id=peer, device_id_type=MESH)

    hbm = (inner_hbm, value_hbm, outer_hbm)
    pieces = [(c, w) for c in range(PARTS) for w in range(3)]

    def mycols(c):
        return pl.ds(pl.multiple_of(par * half + c * part, part), part)

    tok_load = pltpu.make_async_copy(tok_hbm, tok.at[0], local_sems.at[0])
    ow_load = pltpu.make_async_copy(outw_hbm, outw.at[0], local_sems.at[1])
    w_load = {
        (c, w): pltpu.make_async_copy(hbm[w].at[:, mycols(c)], wts.at[c, w, 0], local_sems.at[2 + i])
        for i, (c, w) in enumerate(pieces)
    }
    tok_load.start()
    for p in pieces:
        w_load[p].start()
    ow_load.start()

    chunks = 2
    crow = seq // 2 // chunks
    trow = [pl.ds(pl.multiple_of(tp * (seq // 2) + c * crow, 8), crow) for c in range(chunks)]
    tok_z = [remote(tok_hbm.at[r], tok.at[1, r], to_z) for r in trow]
    tok_t = [remote(tok.at[1, r], tok.at[1, r], to_t) for r in trow]
    low, high = pl.ds(0, hrows), pl.ds(hrows, hrows)
    w_x, w_y, d_x, d_y = {}, {}, {}, {}
    for c, w in pieces:
        src = hbm[w].at[:, mycols(c)]
        w_x[c, w] = remote(src, wts.at[c, w, 1], to_x)
        w_y[c, w] = remote(src, wts.at[c, w, 2], to_y)
        d_x[c, w] = remote(wts.at[c, w, 2, low], wts.at[c, w, 3, low], to_x)
        d_y[c, w] = remote(wts.at[c, w, 1, high], wts.at[c, w, 3, high], to_y)
    one = pl.ds(pl.multiple_of(par * hrows, hrows), hrows)
    two = pl.ds(pl.multiple_of((1 - par) * hrows, hrows), hrows)
    o_y = remote(outw_hbm.at[one], outw.at[2, one], to_y)
    o_x = remote(outw_hbm.at[two], outw.at[1, two], to_x)
    oz_y = remote(outw.at[2, one], outw.at[2, one], to_z)
    oz_x = remote(outw.at[1, two], outw.at[1, two], to_z)
    od_x = remote(outw.at[2, one], outw.at[3, one], to_x)
    od_y = remote(outw.at[1, two], outw.at[3, two], to_y)
    group, other = tp * 2 + par, tp * 2 + 1 - par
    peer_group, peer_other = (1 - tp) * 2 + par, (1 - tp) * 2 + 1 - par
    g_z = [remote(mine.at[c], gat.at[group, c], to_z) for c in range(PARTS)]
    g_t = [remote(gat.at[group, c], gat.at[group, c], to_t) for c in range(PARTS)]
    g_f = [remote(gat.at[other, c], gat.at[other, c], to_t) for c in range(PARTS)]

    pl.semaphore_wait(barrier, 4)
    for r in range(chunks):
        tok_z[r].start()
    for w in range(3):
        w_x[0, w].start()
        w_y[0, w].start()

    tile = 128

    def norm(s):
        @pl.loop(0, seq // tile)
        def _(b):
            r = pl.multiple_of(b * tile, tile)
            xf = tok[s, pl.ds(r, tile), :].astype(F32)
            scale = lax.rsqrt(jnp.mean(xf * xf, axis=-1, keepdims=True) + 1e-06)
            y = (xf * scale * gain_ref[...]).astype(BF16)
            for j in range(4):
                nm[j, pl.ds(s * seq + r, tile), :] = y[:, j * rows : (j + 1) * rows]

    mt = 256

    def project(c, w, slots, start, length, fresh):
        @pl.loop(0, length // mt)
        def _(b):
            r = pl.ds(pl.multiple_of(start + b * mt, mt), mt)
            total = None
            for s in slots:
                d = jnp.dot(nm[shard[s], r, :], wts[c, w, s], preferred_element_type=F32)
                total = d if total is None else total + d
            if fresh:
                acc[c, w, r, :] = total
            else:
                acc[c, w, r, :] += total

    prod[0:8, :] = jnp.zeros((8, part), F32)

    def gate(c, s, store):
        tcols = pl.ds(pl.multiple_of(tp * cols + par * half + c * part, part), part)

        @pl.loop(0, seq // tile)
        def _(b):
            r = pl.multiple_of(b * tile, tile)
            a = pl.ds(s * seq + r, tile)
            inner = acc[c, 0, a, :].astype(BF16).astype(F32)
            value = acc[c, 1, a, :].astype(BF16).astype(F32)
            outer = acc[c, 2, a, :].astype(BF16).astype(F32)
            prod[pl.ds(r + 8, tile), :] = inner * value
            window = prod[pl.ds(r, tile + 8), :]
            conv = jnp.zeros((tile, part), F32)
            for k in range(count):
                lo = 8 - (count - 1) + k
                conv = conv + taps_ref[k : k + 1, tcols] * window[lo : lo + tile, :]
            store(pl.ds(r, tile), (outer * conv).astype(BF16))

    def keep_partner(c):
        def store(r, x):
            mine[c, r, :] = x
        return store

    def keep_own(c):
        def store(r, x):
            gat[group, c, r, :] = x
        return store

    tok_load.wait()
    norm(0)
    for w in range(3):
        w_load[0, w].wait()
        w_y[0, w].wait_recv()
        d_x[0, w].start()
        w_x[0, w].wait_recv()
        d_y[0, w].start()
        if w == 2:
            o_y.start()
            o_x.start()
            for v in range(3):
                w_x[1, v].start()
                w_y[1, v].start()
        project(0, w, (0, 1, 2), 0, seq, True)
    tok_z[0].wait_recv()
    tok_t[0].start()
    for w in range(3):
        d_x[0, w].wait_recv()
        d_y[0, w].wait_recv()
        project(0, w, (3,), 0, seq, False)
    for w in range(3):
        w_load[1, w].wait()
        project(1, w, (0,), 0, seq, True)
    tok_z[1].wait_recv()
    tok_t[1].start()
    o_y.wait_recv()
    oz_y.start()
    o_x.wait_recv()
    oz_x.start()
    gate(0, 0, keep_own(0))
    tok_t[0].wait_recv()
    tok_t[1].wait_recv()
    norm(1)
    g_t[0].start()
    for w in range(3):
        project(0, w, (0, 1, 2, 3), seq, seq, True)
    w_y[1, 0].wait_recv()
    d_x[1, 0].start()
    w_x[1, 0].wait_recv()
    d_y[1, 0].start()
    gate(0, 1, keep_partner(0))
    for w in range(3):
        if w > 0:
            w_y[1, w].wait_recv()
            d_x[1, w].start()
            w_x[1, w].wait_recv()
            d_y[1, w].start()
        else:
            project(1, w, (1, 2), 0, seq, False)
            g_z[0].start()
        if w == 2:
            od_x.start()
            od_y.start()
        if w > 0:
            project(1, w, (1, 2), 0, seq, False)
        project(1, w, (0, 1, 2), seq, seq, True)
    for w in range(3):
        d_x[1, w].wait_recv()
        d_y[1, w].wait_recv()
        project(1, w, (3,), seq, seq, False)
        if w < 2:
            project(1, w, (3,), 0, seq, False)
    gate(1, 1, keep_partner(1))
    project(1, 2, (3,), 0, seq, False)
    g_z[1].start()
    gate(1, 0, keep_own(1))
    g_z[0].wait_recv()
    g_f[0].start()
    g_t[0].wait_recv()
    oz_y.wait_recv()
    oz_x.wait_recv()
    ow_load.wait()
    g_t[1].start()
    g_f[0].wait_recv()

    def slot(g):
        return lax.rem(g + fs, 2) + 2 * lax.rem(g // 2 + fs // 2, 2)

    def mix(terms, first, last):
        @pl.loop(0, seq // mt)
        def _(b):
            r = pl.ds(pl.multiple_of(b * mt, mt), mt)
            total = None
            for g, s, c in terms:
                d = jnp.dot(
                    gat[g, c, r, :], outw[s, c * part : (c + 1) * part, :],
                    preferred_element_type=F32,
                )
                total = d if total is None else total + d
            if not first:
                total = total + osum[r, :]
            if last:
                out_ref[r, :] = total.astype(BF16)
            else:
                osum[r, :] = total

    mix([(shard[s], s, 0) for s in range(3)], True, False)
    od_x.wait_recv()
    od_y.wait_recv()
    g_t[1].wait_recv()
    mix([(fd, 3, 0), (group, slot(group), 1), (peer_group, slot(peer_group), 1)], False, False)
    g_z[1].wait_recv()
    g_f[1].start()
    g_f[1].wait_recv()
    mix([(other, slot(other), 1), (peer_other, slot(peer_other), 1)], False, True)

    sent = tok_z + tok_t + [o_x, o_y, oz_x, oz_y, od_x, od_y] + g_z + g_t + g_f
    for p in pieces:
        sent += [w_x[p], w_y[p], d_x[p], d_y[p]]
    for c in sent:
        c.wait_send()


PARTS = 2
COPIES = 40


def paired(tokens, norm_gain, outer_weight, inner_weight, value_weight, conv_taps, out_weight):
    _, seq, width = tokens.shape
    rows, cols = outer_weight.shape
    half = cols // 2
    anyspace = pl.BlockSpec(memory_space=pl.ANY)
    vmem = pl.BlockSpec(memory_space=pltpu.VMEM)
    out = pl.pallas_call(
        kernel,
        out_shape=jax.ShapeDtypeStruct((seq, cols), BF16),
        in_specs=[anyspace, vmem, anyspace, anyspace, anyspace, vmem, anyspace],
        out_specs=vmem,
        scratch_shapes=[
            pltpu.VMEM((2, seq, width), BF16),
            pltpu.VMEM((4, 2 * seq, rows), BF16),
            pltpu.VMEM((PARTS, 3, 4, rows, half // PARTS), BF16),
            pltpu.VMEM((4, rows, cols), BF16),
            pltpu.VMEM((PARTS, 3, 2 * seq, half // PARTS), F32),
            pltpu.VMEM((seq + 8, half // PARTS), F32),
            pltpu.VMEM((4, PARTS, seq, half // PARTS), BF16),
            pltpu.VMEM((PARTS, seq, half // PARTS), BF16),
            pltpu.VMEM((seq, cols), F32),
            pltpu.SemaphoreType.DMA((COPIES,)),
            pltpu.SemaphoreType.DMA((COPIES,)),
            pltpu.SemaphoreType.DMA((2 + 3 * PARTS,)),
        ],
        compiler_params=pltpu.CompilerParams(
            collective_id=0, has_side_effects=True, vmem_limit_bytes=60 * 1024 * 1024
        ),
        name="mixer",
    )(
        tokens.reshape(seq, width), norm_gain.reshape(1, width), outer_weight, inner_weight,
        value_weight, conv_taps, out_weight,
    )
    return out.reshape(1, seq, cols)


def solution(mesh):
    shape = dict(mesh.shape)

    def local(tokens, *rest):
        rows, cols = rest[1].shape
        fits = (
            shape["fs"] == 4 and shape["tp"] == 2 and shape["rep"] % 2 == 0
            and tokens.shape[0] == 1 and tokens.shape[1] % 256 == 0
            and rows % 256 == 0 and cols == 2 * rows and rest[4].shape[0] <= 9
        )
        return (paired if fits else plain)(tokens, *rest)

    in_specs = (
        P(("rep", "fs"), None, None),
        P(),
        P("fs", "tp"),
        P("fs", "tp"),
        P("fs", "tp"),
        P(),
        P("fs", "tp"),
    )
    out_specs = P(("rep", "fs"), None, "tp")
    return jax.shard_map(local, mesh=mesh, in_specs=in_specs, out_specs=out_specs, check_vma=False)
```

```python
import functools

import jax
import jax.numpy as jnp
from jax import lax
from jax.experimental import pallas as pl
from jax.experimental.pallas import tpu as pltpu
from jax.sharding import PartitionSpec as P

MESH = pl.DeviceIdType.MESH
F32 = jnp.float32
BF16 = jnp.bfloat16


def plain(tokens, norm_gain, outer_weight, inner_weight, value_weight, conv_taps, out_weight):
    batch, seq_len, width = tokens.shape
    xf = tokens.astype(F32)
    scale = lax.rsqrt(jnp.mean(xf * xf, axis=-1, keepdims=True) + 1e-06)
    normed = (xf * scale * norm_gain).astype(BF16).reshape(batch * seq_len, width)
    columns = outer_weight.shape[1]

    def project(weight):
        full = lax.all_gather(weight, "fs", axis=0, tiled=True)
        return jnp.dot(normed, full, preferred_element_type=F32).astype(BF16).astype(F32)

    outer, inner, value = project(outer_weight), project(inner_weight), project(value_weight)
    product = (inner * value).reshape(batch, seq_len, columns)
    offset = lax.axis_index("tp") * columns
    taps = lax.dynamic_slice_in_dim(conv_taps, offset, columns, 1)
    count = conv_taps.shape[0]
    padded = jnp.pad(product, ((0, 0), (count - 1, 0), (0, 0)))
    convolved = jnp.zeros((batch, seq_len, columns), F32)
    for k in range(count):
        convolved = convolved + taps[k] * padded[:, k : k + seq_len, :]
    gated = (outer * convolved.reshape(batch * seq_len, columns)).astype(BF16)
    everything = lax.all_gather(gated, "tp", axis=1, tiled=True)
    full = lax.all_gather(out_weight, "fs", axis=0, tiled=True)
    result = jnp.dot(everything, full, preferred_element_type=F32)
    return result.astype(BF16).reshape(batch, seq_len, columns)


def kernel(
    tok_hbm, gain_ref, outer_hbm, inner_hbm, value_hbm, taps_ref, outw_hbm, out_ref,
    tok, nm, wts, outw, acc, prod, gat, mine, osum, send_sems, recv_sems, local_sems,
):
    rep, fs, tp = lax.axis_index("rep"), lax.axis_index("fs"), lax.axis_index("tp")
    seq, width = tok_hbm.shape
    rows, cols = outer_hbm.shape
    half = cols // 2
    part = half // PARTS
    hrows = rows // 2
    count = taps_ref.shape[0]
    par = lax.rem(rep, 2)
    fx = fs + 1 - 2 * lax.rem(fs, 2)
    fy = lax.rem(fs + 2, 4)
    fd = 3 - fs
    shard = (fs, fx, fy, fd)
    to_x, to_y = (rep, fx, tp), (rep, fy, tp)
    to_z, to_t = (rep + 1 - 2 * par, fs, tp), (rep, fs, 1 - tp)
    used = [0]

    def remote(src, dst, device):
        k = used[0]
        used[0] += 1
        return pltpu.make_async_remote_copy(
            src_ref=src, dst_ref=dst, send_sem=send_sems.at[k], recv_sem=recv_sems.at[k],
            device_id=device, device_id_type=MESH,
        )

    barrier = pltpu.get_barrier_semaphore()
    for peer in (to_x, to_y, to_z, to_t):
        pl.semaphore_signal(barrier, inc=1, device_id=peer, device_id_type=MESH)

    hbm = (inner_hbm, value_hbm, outer_hbm)
    pieces = [(c, w) for c in range(PARTS) for w in range(3)]

    def mycols(c):
        return pl.ds(pl.multiple_of(par * half + c * part, part), part)

    tok_load = pltpu.make_async_copy(tok_hbm, tok.at[0], local_sems.at[0])
    ow_load = pltpu.make_async_copy(outw_hbm, outw.at[0], local_sems.at[1])
    w_load = {
        (c, w): pltpu.make_async_copy(hbm[w].at[:, mycols(c)], wts.at[c, w, 0], local_sems.at[2 + i])
        for i, (c, w) in enumerate(pieces)
    }
    tok_load.start()
    for p in pieces:
        w_load[p].start()
    ow_load.start()

    chunks = 2
    crow = seq // 2 // chunks
    trow = [pl.ds(pl.multiple_of(tp * (seq // 2) + c * crow, 8), crow) for c in range(chunks)]
    tok_z = [remote(tok_hbm.at[r], tok.at[1, r], to_z) for r in trow]
    tok_t = [remote(tok.at[1, r], tok.at[1, r], to_t) for r in trow]
    low, high = pl.ds(0, hrows), pl.ds(hrows, hrows)
    w_x, w_y, d_x, d_y = {}, {}, {}, {}
    for c, w in pieces:
        src = hbm[w].at[:, mycols(c)]
        w_x[c, w] = remote(src, wts.at[c, w, 1], to_x)
        w_y[c, w] = remote(src, wts.at[c, w, 2], to_y)
        d_x[c, w] = remote(wts.at[c, w, 2, low], wts.at[c, w, 3, low], to_x)
        d_y[c, w] = remote(wts.at[c, w, 1, high], wts.at[c, w, 3, high], to_y)
    one = pl.ds(pl.multiple_of(par * hrows, hrows), hrows)
    two = pl.ds(pl.multiple_of((1 - par) * hrows, hrows), hrows)
    o_y = remote(outw_hbm.at[one], outw.at[2, one], to_y)
    o_x = remote(outw_hbm.at[two], outw.at[1, two], to_x)
    oz_y = remote(outw.at[2, one], outw.at[2, one], to_z)
    oz_x = remote(outw.at[1, two], outw.at[1, two], to_z)
    od_x = remote(outw.at[2, one], outw.at[3, one], to_x)
    od_y = remote(outw.at[1, two], outw.at[3, two], to_y)
    group, other = tp * 2 + par, tp * 2 + 1 - par
    peer_group, peer_other = (1 - tp) * 2 + par, (1 - tp) * 2 + 1 - par
    g_z = [remote(mine.at[c], gat.at[group, c], to_z) for c in range(PARTS)]
    g_t = [remote(gat.at[group, c], gat.at[group, c], to_t) for c in range(PARTS)]
    g_f = [remote(gat.at[other, c], gat.at[other, c], to_t) for c in range(PARTS)]

    pl.semaphore_wait(barrier, 4)
    for r in range(chunks):
        tok_z[r].start()
    for w in range(3):
        w_x[0, w].start()
        w_y[0, w].start()
    o_y.start()
    o_x.start()

    tile = 128

    def norm(s):
        @pl.loop(0, seq // tile)
        def _(b):
            r = pl.multiple_of(b * tile, tile)
            xf = tok[s, pl.ds(r, tile), :].astype(F32)
            scale = lax.rsqrt(jnp.mean(xf * xf, axis=-1, keepdims=True) + 1e-06)
            y = (xf * scale * gain_ref[...]).astype(BF16)
            for j in range(4):
                nm[j, pl.ds(s * seq + r, tile), :] = y[:, j * rows : (j + 1) * rows]

    mt = 256

    def project(c, w, slots, start, length, fresh):
        @pl.loop(0, length // mt)
        def _(b):
            r = pl.ds(pl.multiple_of(start + b * mt, mt), mt)
            total = None
            for s in slots:
                d = jnp.dot(nm[shard[s], r, :], wts[c, w, s], preferred_element_type=F32)
                total = d if total is None else total + d
            if fresh:
                acc[c, w, r, :] = total
            else:
                acc[c, w, r, :] += total

    prod[0:8, :] = jnp.zeros((8, part), F32)

    def gate(c, s, store):
        tcols = pl.ds(pl.multiple_of(tp * cols + par * half + c * part, part), part)

        @pl.loop(0, seq // tile)
        def _(b):
            r = pl.multiple_of(b * tile, tile)
            a = pl.ds(s * seq + r, tile)
            inner = acc[c, 0, a, :].astype(BF16).astype(F32)
            value = acc[c, 1, a, :].astype(BF16).astype(F32)
            outer = acc[c, 2, a, :].astype(BF16).astype(F32)
            prod[pl.ds(r + 8, tile), :] = inner * value
            window = prod[pl.ds(r, tile + 8), :]
            conv = jnp.zeros((tile, part), F32)
            for k in range(count):
                lo = 8 - (count - 1) + k
                conv = conv + taps_ref[k : k + 1, tcols] * window[lo : lo + tile, :]
            store(pl.ds(r, tile), (outer * conv).astype(BF16))

    def keep_partner(c):
        def store(r, x):
            mine[c, r, :] = x
        return store

    def keep_own(c):
        def store(r, x):
            gat[group, c, r, :] = x
        return store

    tok_load.wait()
    norm(0)
    for w in range(3):
        w_load[0, w].wait()
        w_y[0, w].wait_recv()
        d_x[0, w].start()
        w_x[0, w].wait_recv()
        d_y[0, w].start()
        if w == 2:
            for v in range(3):
                w_x[1, v].start()
                w_y[1, v].start()
        project(0, w, (0, 1, 2), 0, seq, True)
    tok_z[0].wait_recv()
    tok_t[0].start()
    for w in range(3):
        w_load[1, w].wait()
        project(1, w, (0,), 0, seq, True)
    o_y.wait_recv()
    oz_y.start()
    o_x.wait_recv()
    oz_x.start()
    tok_z[1].wait_recv()
    tok_t[1].start()
    for w in range(3):
        d_x[0, w].wait_recv()
        d_y[0, w].wait_recv()
        project(0, w, (3,), 0, seq, False)
    gate(0, 0, keep_own(0))
    tok_t[0].wait_recv()
    tok_t[1].wait_recv()
    norm(1)
    g_t[0].start()
    for w in range(3):
        project(0, w, (0, 1, 2, 3), seq, seq, True)
    w_y[1, 0].wait_recv()
    d_x[1, 0].start()
    w_x[1, 0].wait_recv()
    d_y[1, 0].start()
    gate(0, 1, keep_partner(0))
    for w in range(3):
        if w > 0:
            w_y[1, w].wait_recv()
            d_x[1, w].start()
            w_x[1, w].wait_recv()
            d_y[1, w].start()
        else:
            project(1, w, (1, 2), 0, seq, False)
            g_z[0].start()
        if w == 2:
            od_x.start()
            od_y.start()
        if w > 0:
            project(1, w, (1, 2), 0, seq, False)
        project(1, w, (0, 1, 2), seq, seq, True)
    for w in range(3):
        d_x[1, w].wait_recv()
        d_y[1, w].wait_recv()
        project(1, w, (3,), seq, seq, False)
        if w < 2:
            project(1, w, (3,), 0, seq, False)
    gate(1, 1, keep_partner(1))
    project(1, 2, (3,), 0, seq, False)
    g_z[1].start()
    gate(1, 0, keep_own(1))
    g_z[0].wait_recv()
    g_f[0].start()
    g_t[0].wait_recv()
    oz_y.wait_recv()
    oz_x.wait_recv()
    ow_load.wait()
    g_t[1].start()
    g_f[0].wait_recv()

    def slot(g):
        return lax.rem(g + fs, 2) + 2 * lax.rem(g // 2 + fs // 2, 2)

    def mix(terms, first, last):
        @pl.loop(0, seq // mt)
        def _(b):
            r = pl.ds(pl.multiple_of(b * mt, mt), mt)
            total = None
            for g, s, c in terms:
                d = jnp.dot(
                    gat[g, c, r, :], outw[s, c * part : (c + 1) * part, :],
                    preferred_element_type=F32,
                )
                total = d if total is None else total + d
            if not first:
                total = total + osum[r, :]
            if last:
                out_ref[r, :] = total.astype(BF16)
            else:
                osum[r, :] = total

    mix([(shard[s], s, 0) for s in range(3)], True, False)
    od_x.wait_recv()
    od_y.wait_recv()
    g_t[1].wait_recv()
    mix([(fd, 3, 0), (group, slot(group), 1), (peer_group, slot(peer_group), 1)], False, False)
    g_z[1].wait_recv()
    g_f[1].start()
    mix([(other, slot(other), 1)], False, False)
    g_f[1].wait_recv()
    mix([(peer_other, slot(peer_other), 1)], False, True)

    sent = tok_z + tok_t + [o_x, o_y, oz_x, oz_y, od_x, od_y] + g_z + g_t + g_f
    for p in pieces:
        sent += [w_x[p], w_y[p], d_x[p], d_y[p]]
    for c in sent:
        c.wait_send()


PARTS = 2
COPIES = 40


def paired(tokens, norm_gain, outer_weight, inner_weight, value_weight, conv_taps, out_weight):
    _, seq, width = tokens.shape
    rows, cols = outer_weight.shape
    half = cols // 2
    anyspace = pl.BlockSpec(memory_space=pltpu.HBM)
    vmem = pl.BlockSpec(memory_space=pltpu.VMEM)
    out = pl.pallas_call(
        kernel,
        out_shape=pltpu.VMEM((seq, cols), BF16),
        in_specs=[anyspace, vmem, anyspace, anyspace, anyspace, vmem, anyspace],
        out_specs=vmem,
        scratch_shapes=[
            pltpu.VMEM((2, seq, width), BF16),
            pltpu.VMEM((4, 2 * seq, rows), BF16),
            pltpu.VMEM((PARTS, 3, 4, rows, half // PARTS), BF16),
            pltpu.VMEM((4, rows, cols), BF16),
            pltpu.VMEM((PARTS, 3, 2 * seq, half // PARTS), F32),
            pltpu.VMEM((seq + 8, half // PARTS), F32),
            pltpu.VMEM((4, PARTS, seq, half // PARTS), BF16),
            pltpu.VMEM((PARTS, seq, half // PARTS), BF16),
            pltpu.VMEM((seq, cols), F32),
            pltpu.SemaphoreType.DMA((COPIES,)),
            pltpu.SemaphoreType.DMA((COPIES,)),
            pltpu.SemaphoreType.DMA((2 + 3 * PARTS,)),
        ],
        compiler_params=pltpu.CompilerParams(
            collective_id=0, has_side_effects=True, vmem_limit_bytes=58 * 1024 * 1024
        ),
        name="mixer",
    )(
        tokens.reshape(seq, width), norm_gain.reshape(1, width), outer_weight, inner_weight,
        value_weight, conv_taps, out_weight,
    )
    return out.reshape(1, seq, cols)


def solution(mesh):
    shape = dict(mesh.shape)

    def local(tokens, *rest):
        rows, cols = rest[1].shape
        fits = (
            shape["fs"] == 4 and shape["tp"] == 2 and shape["rep"] % 2 == 0
            and tokens.shape[0] == 1 and tokens.shape[1] % 256 == 0
            and rows % 256 == 0 and cols == 2 * rows and rest[4].shape[0] <= 9
        )
        return (paired if fits else plain)(tokens, *rest)

    in_specs = (
        P(("rep", "fs"), None, None),
        P(),
        P("fs", "tp"),
        P("fs", "tp"),
        P("fs", "tp"),
        P(),
        P("fs", "tp"),
    )
    out_specs = P(("rep", "fs"), None, "tp")
    return jax.shard_map(local, mesh=mesh, in_specs=in_specs, out_specs=out_specs, check_vma=False)
```
